32 devices in a mesh: ep: 8 (over z, y), tp: 4 (over x, core).
Axes of the slice: x: 2, y: 2, z: 4, core: 2. Of those that a mesh axis runs over, the one named last changes fastest.
Arguments:
- tokens: bfloat16 [1344, 2048], P('ep'), may hold values from -6 to 6
- cotangent: bfloat16 [1344, 2048], P('ep'), may hold values from -6 to 6
- group_ids: int32 [1344, 1], P('ep'), may hold values from 0 to 7; in each aligned block of 168 rows (0 to 167, 168 to 335, ...) at most 32 rows name the same one
- within_ids: int32 [1344, 2], P('ep'), may hold values from 0 to 1, all different within a row
- gate_weights: bfloat16 [1344, 2], P('ep'), may hold values from 0.099609375 to 1
- w_gate: bfloat16 [16, 2048, 1024], P('ep', None, 'tp'), may hold values from -0.125 to 0.125
- w_up: bfloat16 [16, 2048, 1024], P('ep', None, 'tp'), may hold values from -0.125 to 0.125
- w_down: bfloat16 [16, 1024, 2048], P('ep', 'tp'), may hold values from -0.1875 to 0.1875
Outputs:
- tokens_grad: bfloat16 [1344, 2048], P('ep', 'tp')
- gate_grad: float32 [1344, 2], P('ep')
- w_gate_grad: bfloat16 [16, 2048, 1024], P('ep', None, 'tp')
- w_up_grad: bfloat16 [16, 2048, 1024], P('ep', None, 'tp')
- w_down_grad: bfloat16 [16, 1024, 2048], P('ep', 'tp')
The draws below stay inside these ranges and needn't reach their ends.
Inputs may be any that keep to these rules, and one draw needn't show every extreme that they name: `group_ids`: in the rows of one device no group is chosen by more than 32 rows. `within_ids`: the two entries of a row differ.
All inputs are finite; a program needn't handle non-finite values.
Results may differ from the reference program's by a relative error of at most 0.017.
Values may be sent and summed in bfloat16 or wider, within the bound.
A program may use at most 64 MiB of HBM per device.

```python
import math
import jax
import jax.numpy as jnp
import numpy as np
from jax import lax

D = 2048
FF = 1024
GROUP_EXPERTS = 2
TOP_K = 2
TOK_DEV = 168
GROUPS = 8
EXPERTS = 16
CAP = 32
TOKENS = 1344
N_EP = 8
N_TP = 4


def steps_of(stream_key, shape, shards, least, largest):
    loudness, own = 1.0, jax.random.fold_in(stream_key, 6)
    for position, shards_of in shards:
        steps = jnp.exp(jax.random.uniform(jax.random.fold_in(own, position), (shards_of,), jnp.float32, least / len(shards), largest / len(shards)))
        loudness = loudness * jnp.repeat(steps, shape[position] // shards_of).reshape([-1 if axis == position else 1 for axis in range(len(shape))])
    return loudness


def different_ones(stream_key, rows, number_of, top, lift):
    ranking = jax.random.permutation(jax.random.fold_in(stream_key, 1), number_of)
    pull = ranking
    for power in range(3):
        pull = pull * pull // number_of
    pull = pull * lift // number_of
    tickets = jax.random.randint(jax.random.fold_in(stream_key, 2), (rows, number_of), 0, 4096) + pull
    sure = jax.random.permutation(jax.random.fold_in(stream_key, 3), rows)[jnp.arange(number_of) % rows]
    tickets = jnp.where(jnp.arange(rows)[:, None] == sure[None, :], 1 << 14, tickets)
    score = tickets * number_of + jnp.arange(number_of)
    return lax.top_k(score.astype(jnp.int32), top)[1].astype(jnp.int32)


def routed_block(rng, own, number, rows, count, top, bound, lean):
    ranking = jax.random.permutation(rng, count)
    packed, usual = portions_of(count, rows * top, bound, lean, True), portions_of(count, rows * top, bound, lean, False)
    places = jnp.arange(count)

    def named(sizes, turn):
        used = int((sizes > 0).sum())
        fixed = max(1, used // 4)
        moved = fixed + (places - fixed + turn * (used - fixed)) % max(1, count - fixed)
        return jnp.zeros((count,), jnp.int32).at[ranking[jnp.where(places < fixed, places, moved)]].set(jnp.asarray(sizes, jnp.int32))

    sizes = jnp.where(number % 4 == 0, named(packed, number // 4), named(usual, number - number // 4 - 1))
    mixed = jax.random.permutation(jax.random.fold_in(own, 3), count)
    source_of, receiver = mixed[0:count // 2 * 2:2], mixed[1:count // 2 * 2:2]
    margin = jnp.minimum(sizes[source_of] - 1, bound - sizes[receiver]) // 2
    margin = jnp.where((source_of == ranking[0]) | (receiver == ranking[0]) | (sizes[receiver] == 0), 0, jnp.maximum(margin, 0))
    moved = jax.random.randint(jax.random.fold_in(own, 4), (count // 2,), 0, 1 << 20) % (margin + 1)
    sizes = sizes.at[source_of].add(-moved).at[receiver].add(moved)
    items = jnp.searchsorted(jnp.cumsum(sizes), jnp.arange(rows * top), side="right").astype(jnp.int32)
    grid = items.reshape(top, rows).T
    grid = grid[jax.random.permutation(jax.random.fold_in(own, 1), rows)]
    turn = jax.random.randint(jax.random.fold_in(own, 2), (rows, 1), 0, top)
    return jnp.take_along_axis(grid, (jnp.arange(top)[None, :] + turn) % top, axis=1)


def portions_of(number_of, total, bound, lean, full):
    loads = [(1 << 20) // math.isqrt(rank ** lean) + 1 for rank in range(1, number_of + 1)]
    largest = bound if full else min(bound, max(-(-total // number_of), total * loads[0] // sum(loads)))
    least = 1 if total - largest >= number_of - 1 else 0
    counts, spare = [largest] + [least] * (number_of - 1), total - largest - least * (number_of - 1)
    while spare > 0:
        free = [i for i in range(1, number_of) if counts[i] < largest] or [i for i in range(1, number_of) if counts[i] < bound]
        mass, remaining = sum([loads[i] for i in free]), spare
        for i in free:
            more = min(bound - counts[i], max(1, remaining * loads[i] // mass), spare)
            counts[i] = counts[i] + more
            spare = spare - more
    return np.array(counts)


def noise(stream_key, dims, spread, bound, pieces=(), kind=jnp.bfloat16):
    gain = steps_of(stream_key, dims, pieces, -0.22, 0.18) if pieces else 1.0
    array = jax.random.normal(stream_key, dims, jnp.float32) * spread * gain
    return jnp.minimum(jnp.maximum(array, -bound), bound).astype(kind)


def setup_inputs(seed: int = 0) -> dict:
    splits = jax.random.split(jax.random.key(seed), 9)
    tokens = noise(splits[0], (TOKENS, D), 1.0, 6.0, ((0, 8),))
    cotangent = noise(splits[1], (TOKENS, D), 1.0, 6.0, ((0, 8),))
    group_ids_keys = jax.random.split(jax.random.fold_in(splits[2], 1), TOKENS // TOK_DEV)
    group_ids_turns = jax.random.permutation(jax.random.fold_in(splits[2], 3), TOKENS // TOK_DEV)
    group_ids = jax.vmap(lambda own, number: routed_block(jax.random.fold_in(splits[2], 2), own, number, TOK_DEV, GROUPS, 1, CAP, 2))(group_ids_keys, group_ids_turns).reshape((TOKENS, 1))
    within_ids = different_ones(splits[3], TOKENS, GROUP_EXPERTS, TOP_K, 8192)
    gate_weights = jnp.clip(jnp.exp(math.log(1.0) - 2.306499 * jax.random.uniform(splits[4], (TOKENS, TOP_K), jnp.float32) ** steps_of(splits[4], (TOKENS, TOP_K), ((0, 8),), -0.2, 0.2)), 0.099609375, 1.0).astype(jnp.bfloat16)
    w_gate = noise(splits[5], (EXPERTS, D, FF), D ** -0.5, 0.125, ((0, 8), (2, 4)))
    w_up = noise(splits[6], (EXPERTS, D, FF), D ** -0.5, 0.125, ((0, 8), (2, 4)))
    w_down = noise(splits[7], (EXPERTS, FF, D), FF ** -0.5, 0.1875, ((0, 8), (1, 4)))
    return {"tokens": tokens, "cotangent": cotangent, "group_ids": group_ids, "within_ids": within_ids, "gate_weights": gate_weights, "w_gate": w_gate, "w_up": w_up, "w_down": w_down}


def reference(tokens, cotangent, group_ids, within_ids, gate_weights, w_gate, w_up, w_down):
    rows_max = N_EP * CAP
    ff_local = FF // N_TP
    group_of = group_ids[:, 0]
    sorted_rows = jnp.argsort(group_of, stable=True).astype(jnp.int32)
    in_group = (group_of[:, None] == jnp.arange(GROUPS, dtype=jnp.int32)[None, :]).astype(jnp.int32)
    group_counts = jnp.sum(in_group, axis=0)
    offsets = jnp.cumsum(group_counts) - group_counts
    local_ids = jnp.arange(GROUP_EXPERTS, dtype=jnp.int32)
    chosen = (within_ids[:, :, None] == local_ids[None, None, :]).astype(jnp.float32)
    combine = jnp.sum(chosen * gate_weights.astype(jnp.float32)[:, :, None], axis=1).astype(jnp.bfloat16)

    def one_group(group_index):
        positions = jnp.arange(rows_max, dtype=jnp.int32)
        is_valid = positions < group_counts[group_index]
        row_ids = sorted_rows[jnp.clip(offsets[group_index] + positions, 0, TOKENS - 1)]
        keep = is_valid[:, None]
        slot_x = jnp.where(keep, tokens[row_ids], jnp.zeros((), jnp.bfloat16))
        slot_dy = jnp.where(keep, cotangent[row_ids], jnp.zeros((), jnp.bfloat16))
        slot_comb = jnp.where(keep, combine[row_ids], jnp.zeros((), jnp.bfloat16))
        first = (group_index * GROUP_EXPERTS).astype(jnp.int32)
        local_gate = lax.dynamic_slice_in_dim(w_gate, first, GROUP_EXPERTS, 0)
        local_up = lax.dynamic_slice_in_dim(w_up, first, GROUP_EXPERTS, 0)
        local_down = lax.dynamic_slice_in_dim(w_down, first, GROUP_EXPERTS, 0)
        dy_float = slot_dy.astype(jnp.float32)
        blocks = jnp.zeros((N_TP, rows_max, D), jnp.float32)
        gate_parts = []
        grads_gate = []
        grads_up = []
        grads_down = []
        for expert in range(GROUP_EXPERTS):
            pre_gate = jnp.dot(slot_x, local_gate[expert], preferred_element_type=jnp.float32)
            pre_up = jnp.dot(slot_x, local_up[expert], preferred_element_type=jnp.float32)
            sig_gate = jax.nn.sigmoid(pre_gate)
            act_b = (pre_gate * sig_gate * pre_up).astype(jnp.bfloat16)
            down = jnp.dot(act_b, local_down[expert], preferred_element_type=jnp.float32)
            gate_parts.append(jnp.sum(dy_float * down, axis=1))
            scaled = (slot_comb[:, expert:expert + 1].astype(jnp.float32) * dy_float).astype(jnp.bfloat16)
            grads_down.append(jnp.dot(act_b.T, scaled, preferred_element_type=jnp.float32).astype(jnp.bfloat16))
            act_grad = jnp.dot(scaled, local_down[expert].T, preferred_element_type=jnp.float32)
            gate_b = (act_grad * pre_up * sig_gate * (1.0 + pre_gate * (1.0 - sig_gate))).astype(jnp.bfloat16)
            up_b = (act_grad * pre_gate * sig_gate).astype(jnp.bfloat16)
            grads_gate.append(jnp.dot(slot_x.T, gate_b, preferred_element_type=jnp.float32).astype(jnp.bfloat16))
            grads_up.append(jnp.dot(slot_x.T, up_b, preferred_element_type=jnp.float32).astype(jnp.bfloat16))
            gate_split = gate_b.astype(jnp.float32).reshape(rows_max, N_TP, ff_local)
            up_split = up_b.astype(jnp.float32).reshape(rows_max, N_TP, ff_local)
            wg_split = local_gate[expert].astype(jnp.float32).reshape(D, N_TP, ff_local)
            wu_split = local_up[expert].astype(jnp.float32).reshape(D, N_TP, ff_local)
            blocks = blocks + jnp.einsum('rnf,dnf->nrd', gate_split, wg_split)
            blocks = blocks + jnp.einsum('rnf,dnf->nrd', up_split, wu_split)
        rounded = lax.optimization_barrier(blocks.astype(jnp.bfloat16)).astype(jnp.float32)
        dx_rows = jnp.sum(rounded, axis=0).astype(jnp.bfloat16)
        return (dx_rows, jnp.stack(gate_parts, axis=1), row_ids, is_valid,
                jnp.stack(grads_gate), jnp.stack(grads_up), jnp.stack(grads_down))

    dx_all, gate_all, rows_all, valid_all, gg_all, gu_all, gd_all = lax.map(
        one_group, jnp.arange(GROUPS, dtype=jnp.int32))
    flat_rows = rows_all.reshape(-1)
    flat_valid = valid_all.reshape(-1)[:, None]
    dx_flat = jnp.where(flat_valid, dx_all.reshape(-1, D).astype(jnp.float32), 0.0)
    tokens_grad = jnp.zeros((TOKENS, D), jnp.float32).at[flat_rows].add(dx_flat).astype(jnp.bfloat16)
    gate_flat = jnp.where(flat_valid, gate_all.reshape(-1, GROUP_EXPERTS), 0.0)
    dense_gate = jnp.zeros((TOKENS, GROUP_EXPERTS), jnp.float32).at[flat_rows].add(gate_flat)
    gate_grad = jnp.sum(chosen * dense_gate[:, None, :], axis=2)
    w_gate_grad = gg_all.reshape(EXPERTS, D, FF)
    w_up_grad = gu_all.reshape(EXPERTS, D, FF)
    w_down_grad = gd_all.reshape(EXPERTS, FF, D)
    return tokens_grad, gate_grad, w_gate_grad, w_up_grad, w_down_grad
```

```python
import functools

import jax
import jax.numpy as jnp
from jax import lax
from jax.experimental import pallas as pl
from jax.experimental.pallas import tpu as pltpu
from jax.sharding import PartitionSpec as P

MESH = pl.DeviceIdType.MESH
LANES = 128
NT = (((1,), (1,)), ((), ()))
TN = (((0,), (0,)), ((), ()))
NN = (((1,), (0,)), ((), ()))


def dot(a, b, dims=NN):
    return lax.dot_general(a, b, dims, preferred_element_type=jnp.float32)


def each(count, body):
    if count <= 8:
        for i in range(count):
            body(i)
    else:
        lax.fori_loop(0, count, lambda i, c: (body(i), c)[1], 0)


def aligned(value, step):
    return value if isinstance(value, int) else pl.multiple_of(value, step)


def kernel(
    ep, tp, cap,
    tok_ref, cot_ref, gid_ref, wid_ref, gw_ref, wg_ref, wu_ref, wd_ref,
    dtok_ref, dgate_ref, gwg_ref, gwu_ref, gwd_ref,
    src, placed, rows_in, wg, wu, wd, acc, gate_b, up_b, act_c,
    to_partner, from_partner, dx_acc, to_x, from_x, to_ep, back,
    gate_in, gate_sum, gate_back, vwg, vwu, vwd,
    load_sem, out_sem, own_sem, send1, recv_rows, send_x, send_p, send_p2,
    dxp_send, dxp_recv, dxx_send, dxx_recv, dxe_send, dxe_recv,
    gt_send, gt_recv, ge_send, ge_recv,
):
    e_me = lax.axis_index("ep")
    t_me = lax.axis_index("tp")
    core = lax.rem(t_me, 2)
    x_me = lax.div(t_me, 2)
    partner = t_me + 1 - 2 * core
    nx = tp // 2
    tok_rows, width = tok_ref.shape
    cs = width // tp
    slots = ep * cap
    experts = wg.shape[0]
    bf16 = jnp.bfloat16

    barrier = pltpu.get_barrier_semaphore()
    each(ep - 1, lambda i: pl.semaphore_signal(
        barrier, inc=1, device_id=(lax.rem(e_me + 1 + i, ep), t_me), device_id_type=MESH))
    each(tp - 1, lambda i: pl.semaphore_signal(
        barrier, inc=1, device_id=(e_me, lax.rem(t_me + 1 + i, tp)), device_id_type=MESH))

    my_cols = pl.ds(pl.multiple_of(t_me * cs, LANES), cs)
    loads = [
        pltpu.make_async_copy(tok_ref.at[:, my_cols], src.at[:, pl.ds(0, cs)], load_sem.at[0]),
        pltpu.make_async_copy(cot_ref.at[:, my_cols], src.at[:, pl.ds(cs, cs)], load_sem.at[1]),
        pltpu.make_async_copy(wg_ref, wg, load_sem.at[2]),
        pltpu.make_async_copy(wu_ref, wu, load_sem.at[3]),
        pltpu.make_async_copy(wd_ref, wd, load_sem.at[4]),
    ]
    for load in loads:
        load.start()

    group = gid_ref[...]
    in_group = (group == lax.broadcasted_iota(jnp.int32, (tok_rows, LANES), 1)).astype(jnp.float32)
    earlier = (
        lax.broadcasted_iota(jnp.int32, (tok_rows, tok_rows), 0)
        > lax.broadcasted_iota(jnp.int32, (tok_rows, tok_rows), 1)
    ).astype(jnp.float32).astype(bf16)
    before = dot(earlier, in_group.astype(bf16))
    rank = jnp.sum(before * in_group, axis=1, keepdims=True).astype(jnp.int32)
    slot_lane = lax.broadcasted_iota(jnp.int32, (tok_rows, slots), 1)
    place = (slot_lane == group * cap + rank).astype(jnp.float32).astype(bf16)
    lane = lax.broadcasted_iota(jnp.int32, (tok_rows, LANES), 1)
    weights = gw_ref[...].astype(jnp.float32)
    comb = jnp.zeros((tok_rows, LANES), jnp.float32)
    for k in range(weights.shape[1]):
        comb = comb + jnp.where(lane == wid_ref[:, k : k + 1], weights[:, k : k + 1], 0.0)
    src[:, pl.ds(2 * cs, LANES)] = comb.astype(bf16)
    loads[0].wait()
    loads[1].wait()
    placed[...] = dot(place, src[...], TN).astype(bf16)

    pl.semaphore_wait(barrier, ep + tp - 2)

    def block(e):
        return pl.ds(aligned(e * cap, 16), cap)

    distances = list(range(ep))
    if ep <= 8:
        distances = [0]
        for k in range(1, ep // 2 + 1):
            distances += sorted({k, ep - k})

    def stage1(d):
        g = lax.rem(e_me + d, ep)
        return pltpu.make_async_remote_copy(
            src_ref=placed.at[block(g)], dst_ref=rows_in.at[t_me, block(e_me)],
            send_sem=send1.at[d], recv_sem=recv_rows.at[t_me, e_me],
            device_id=(g, t_me), device_id_type=MESH)

    own = pltpu.make_async_copy(
        placed.at[block(e_me)], rows_in.at[t_me, block(e_me)], own_sem.at[0])
    own.start()
    if ep <= 8:
        for d in distances[1:]:
            stage1(d).start()
    else:
        each(ep - 1, lambda i: stage1(i + 1).start())

    def arrived(q, e, cols):
        part = rows_in.at[q, block(e), pl.ds(0, cols)]
        pltpu.make_async_remote_copy(
            src_ref=part, dst_ref=part, send_sem=send1.at[0], recv_sem=recv_rows.at[q, e],
            device_id=(e_me, partner), device_id_type=MESH).wait_recv()

    def forward(q, e, sem, target):
        part = rows_in.at[q, block(e), pl.ds(0, 2 * cs)]
        return pltpu.make_async_remote_copy(
            src_ref=part, dst_ref=part, send_sem=sem, recv_sem=recv_rows.at[q, e],
            device_id=(e_me, target), device_id_type=MESH)

    def x_peer(k):
        return lax.rem(x_me + k, nx) * 2 + core

    def to_peers(d):
        e = lax.rem(e_me - d + ep, ep)
        copies = [forward(t_me, e, send_x.at[k - 1, d], x_peer(k)) for k in range(1, nx)]
        return copies + [forward(t_me, e, send_p.at[d], partner)]

    def stage2(d):
        for copy in to_peers(d):
            copy.start()

    def relays(d):
        e = lax.rem(e_me - d + ep, ep)
        return [(x_peer(k), e, forward(x_peer(k), e, send_p2.at[k - 1, d], partner))
                for k in range(1, nx)]

    def stage3(d):
        for q, e, copy in relays(d):
            arrived(q, e, 2 * cs)
            copy.start()

    own.wait()
    stage2(0)
    if ep <= 8:
        for i, d in enumerate(distances[1:]):
            arrived(t_me, lax.rem(e_me - d + ep, ep), 2 * cs + LANES)
            stage2(d)
            stage3(distances[i])
    else:
        def later(i):
            arrived(t_me, lax.rem(e_me - i - 1 + ep, ep), 2 * cs + LANES)
            stage2(i + 1)
        each(ep - 1, later)
        each(ep - 1, stage3)

    for load in loads[2:]:
        load.wait()

    def share(q):
        return pl.ds(aligned(q * cs, LANES), cs)

    def hidden(q, first):
        xq = rows_in[q, :, pl.ds(0, cs)]
        yq = rows_in[q, :, pl.ds(cs, cs)]
        for e in range(experts):
            for n, value in enumerate((
                dot(xq, wg[e, share(q), :]),
                dot(xq, wu[e, share(q), :]),
                dot(yq, wd[e, :, share(q)], NT),
            )):
                acc[e, n] = value if first else acc[e, n] + value

    def all_arrived(q):
        each(ep, lambda e: arrived(q, e, 2 * cs))

    hidden(t_me, True)
    stage3(distances[-1])
    all_arrived(partner)
    hidden(partner, False)

    def x_quarters(k):
        hidden(x_peer(k), False)
        other = lax.rem(x_me + k, nx) * 2 + 1 - core
        all_arrived(other)
        hidden(other, False)
    each(nx - 1, lambda i: x_quarters(i + 1))

    row8 = lax.broadcasted_iota(jnp.int32, (8, slots), 0)
    gates = jnp.zeros((8, slots), jnp.float32)
    for e in range(experts):
        pre_gate, pre_up, dy_down = acc[e, 0], acc[e, 1], acc[e, 2]
        c = rows_in[t_me, :, pl.ds(2 * cs, LANES)][:, e : e + 1].astype(jnp.float32)
        sig = jax.nn.sigmoid(pre_gate)
        silu = pre_gate * sig
        act = silu * pre_up
        prod = act.astype(bf16).astype(jnp.float32) * dy_down
        act_grad = c * dy_down
        act_c[e] = (c * act).astype(bf16)
        gate_b[e] = (act_grad * pre_up * sig * (1.0 + pre_gate * (1.0 - sig))).astype(bf16)
        up_b[e] = (act_grad * silu).astype(bf16)
        high = prod.astype(bf16)
        low = (prod - high.astype(jnp.float32)).astype(bf16)
        ones = jnp.ones((8, prod.shape[1]), bf16)
        gates = gates + jnp.where(row8 == e, dot(ones, high, NT) + dot(ones, low, NT), 0.0)
    gate_in[t_me] = gates

    def gate_tp(i):
        return pltpu.make_async_remote_copy(
            src_ref=gate_in.at[t_me], dst_ref=gate_in.at[t_me],
            send_sem=gt_send.at[i], recv_sem=gt_recv.at[t_me],
            device_id=(e_me, lax.rem(t_me + 1 + i, tp)), device_id_type=MESH)

    def dx_of(q):
        total = None
        for e in range(experts):
            part = dot(gate_b[e], wg[e, share(q), :], NT) + dot(up_b[e], wu[e, share(q), :], NT)
            total = part if total is None else total + part
        return total

    def dx_partner(k):
        return pltpu.make_async_remote_copy(
            src_ref=to_partner.at[k], dst_ref=from_partner.at[k],
            send_sem=dxp_send.at[k], recv_sem=dxp_recv.at[k],
            device_id=(e_me, partner), device_id_type=MESH)

    def give_partner(i):
        k = nx - 1 - i
        to_partner[k] = dx_of(lax.rem(x_me + k, nx) * 2 + 1 - core).astype(bf16)
        dx_partner(k).start()
    each(nx, give_partner)
    each(tp - 1, lambda i: gate_tp(i).start())

    def dx_x(k, d):
        e = lax.rem(e_me + d, ep)
        return pltpu.make_async_remote_copy(
            src_ref=to_x.at[k - 1, block(e)], dst_ref=from_x.at[k - 1, block(e)],
            send_sem=dxx_send.at[k - 1, d], recv_sem=dxx_recv.at[k - 1, d],
            device_id=(e_me, x_peer(k)), device_id_type=MESH)

    far = distances[::-1]

    def walk(body):
        if ep <= 8:
            for i, d in enumerate(far):
                body(i, d)
        else:
            each(ep, lambda i: body(i, ep - 1 - i))

    def give_x(k):
        mine = dx_of(x_peer(k))
        dx_partner(k).wait_recv()
        to_x[k - 1] = (mine + from_partner[k].astype(jnp.float32)).astype(bf16)
        walk(lambda i, d: dx_x(k, d).start())
    each(nx - 1, lambda i: give_x(i + 1))
    mine = dx_of(t_me)
    dx_partner(0).wait_recv()
    dx_acc[...] = mine + from_partner[0].astype(jnp.float32)

    def gate_ep(d):
        return pltpu.make_async_remote_copy(
            src_ref=gate_sum, dst_ref=gate_back.at[e_me],
            send_sem=ge_send.at[d], recv_sem=ge_recv.at[e_me],
            device_id=(lax.rem(e_me + d, ep), t_me), device_id_type=MESH)

    def gate_wait(i):
        q = lax.rem(t_me + 1 + i, tp)
        pltpu.make_async_remote_copy(
            src_ref=gate_in.at[q], dst_ref=gate_in.at[q],
            send_sem=gt_send.at[i], recv_sem=gt_recv.at[q],
            device_id=(e_me, q), device_id_type=MESH).wait_recv()
    each(tp - 1, gate_wait)
    total = gate_in[0]
    for q in range(1, tp):
        total = total + gate_in[q]
    gate_sum[...] = total
    gate_back[e_me] = total
    each(ep - 1, lambda i: gate_ep(i + 1).start())

    def outs(q):
        cols = share(q)
        return [
            pltpu.make_async_copy(vwg.at[:, cols, :], gwg_ref.at[:, cols, :], out_sem.at[q, 0]),
            pltpu.make_async_copy(vwu.at[:, cols, :], gwu_ref.at[:, cols, :], out_sem.at[q, 1]),
            pltpu.make_async_copy(vwd.at[:, :, cols], gwd_ref.at[:, :, cols], out_sem.at[q, 2]),
        ]

    def weight_grads(q):
        x_t = rows_in[q, :, pl.ds(0, cs)].T
        yq = rows_in[q, :, pl.ds(cs, cs)]
        for e in range(experts):
            vwg[e, share(q), :] = dot(x_t, gate_b[e]).astype(bf16)
            vwu[e, share(q), :] = dot(x_t, up_b[e]).astype(bf16)
            vwd[e, :, share(q)] = dot(act_c[e], yq, TN).astype(bf16)
        for copy in outs(q):
            copy.start()

    def dx_ep(d):
        g = lax.rem(e_me + d, ep)
        return pltpu.make_async_remote_copy(
            src_ref=to_ep.at[block(g)], dst_ref=back.at[block(e_me)],
            send_sem=dxe_send.at[d], recv_sem=dxe_recv.at[e_me],
            device_id=(g, t_me), device_id_type=MESH)

    def finish_chunk(d):
        rows = block(lax.rem(e_me + d, ep))
        value = dx_acc[rows, :]
        for k in range(1, nx):
            dx_x(k, d).wait_recv()
            value = value + from_x[k - 1, rows, :].astype(jnp.float32)
        return value.astype(bf16)

    def chunk(i, d):
        to_ep[block(lax.rem(e_me + d, ep)), :] = finish_chunk(d)
        dx_ep(d).start()

    if ep <= 8:
        done = 0
        for i, d in enumerate(far[:-1]):
            chunk(i, d)
            if i % 2 == 0 and done < tp:
                weight_grads(done)
                done += 1
        for q in range(done, tp):
            weight_grads(q)
    else:
        each(ep - 1, lambda i: chunk(i, ep - 1 - i))
        each(tp, weight_grads)
    back[block(e_me), :] = finish_chunk(0)

    def gate_arrived(i):
        g = lax.rem(e_me + 1 + i, ep)
        pltpu.make_async_remote_copy(
            src_ref=gate_sum, dst_ref=gate_back.at[g],
            send_sem=ge_send.at[0], recv_sem=ge_recv.at[g],
            device_id=(g, t_me), device_id_type=MESH).wait_recv()
    each(ep - 1, gate_arrived)
    pick = (slot_lane == e_me * cap + rank).astype(jnp.float32).astype(bf16)
    sums = gate_back[...].reshape(ep * 8, slots)
    high = sums.astype(bf16)
    low = (sums - high.astype(jnp.float32)).astype(bf16)
    dense = dot(pick, high, NT) + dot(pick, low, NT)
    row_lane = lax.broadcasted_iota(jnp.int32, (tok_rows, ep * 8), 1)
    for k in range(weights.shape[1]):
        wanted = row_lane == group * 8 + wid_ref[:, k : k + 1]
        dgate_ref[:, k : k + 1] = jnp.sum(jnp.where(wanted, dense, 0.0), axis=1, keepdims=True)

    def back_arrived(i):
        g = lax.rem(e_me + 1 + i, ep)
        pltpu.make_async_remote_copy(
            src_ref=to_ep.at[block(g)], dst_ref=back.at[block(g)],
            send_sem=dxe_send.at[0], recv_sem=dxe_recv.at[g],
            device_id=(g, t_me), device_id_type=MESH).wait_recv()
    each(ep - 1, back_arrived)
    dtok_ref[...] = dot(place, back[...]).astype(bf16)

    def sent1(i):
        d = i + 1
        stage1(d).wait_send()
        gate_ep(d).wait_send()
        dx_ep(d).wait_send()
    each(ep - 1, sent1)

    def sent2(d):
        for copy in to_peers(d):
            copy.wait_send()
        for _, _, copy in relays(d):
            copy.wait_send()
        for k in range(1, nx):
            dx_x(k, d).wait_send()
    each(ep, sent2)
    each(nx, lambda k: dx_partner(k).wait_send())
    each(tp - 1, lambda i: gate_tp(i).wait_send())

    def written(q):
        for copy in outs(q):
            copy.wait()
    each(tp, written)


def on_device(tokens, cotangent, group_ids, within_ids, gate_weights, w_gate, w_up, w_down):
    ep = lax.axis_size("ep")
    tp = lax.axis_size("tp")
    tok_rows, width = tokens.shape
    experts, _, ff = w_gate.shape
    cap = (3 * tok_rows + 2 * ep - 1) // (2 * ep)
    cap = -(-cap // 16) * 16
    slots = ep * cap
    cs = width // tp
    nx = tp // 2
    bf16, f32 = jnp.bfloat16, jnp.float32
    dma = pltpu.SemaphoreType.DMA
    anywhere = pl.BlockSpec(memory_space=pl.ANY)
    vmem = pl.BlockSpec(memory_space=pltpu.VMEM)
    scratch = [
        pltpu.VMEM((tok_rows, 2 * cs + LANES), bf16),
        pltpu.VMEM((slots, 2 * cs + LANES), bf16),
        pltpu.VMEM((tp, slots, 2 * cs + LANES), bf16),
        pltpu.VMEM(w_gate.shape, bf16),
        pltpu.VMEM(w_up.shape, bf16),
        pltpu.VMEM(w_down.shape, bf16),
        pltpu.VMEM((experts, 3, slots, ff), f32),
        pltpu.VMEM((experts, slots, ff), bf16),
        pltpu.VMEM((experts, slots, ff), bf16),
        pltpu.VMEM((experts, slots, ff), bf16),
        pltpu.VMEM((nx, slots, cs), bf16),
        pltpu.VMEM((nx, slots, cs), bf16),
        pltpu.VMEM((slots, cs), f32),
        pltpu.VMEM((nx - 1, slots, cs), bf16),
        pltpu.VMEM((nx - 1, slots, cs), bf16),
        pltpu.VMEM((slots, cs), bf16),
        pltpu.VMEM((slots, cs), bf16),
        pltpu.VMEM((tp, 8, slots), f32),
        pltpu.VMEM((8, slots), f32),
        pltpu.VMEM((ep, 8, slots), f32),
        pltpu.VMEM(w_gate.shape, bf16),
        pltpu.VMEM(w_up.shape, bf16),
        pltpu.VMEM(w_down.shape, bf16),
        dma((5,)), dma((tp, 3)), dma((1,)), dma((ep,)), dma((tp, ep)),
        dma((nx - 1, ep)), dma((ep,)), dma((nx - 1, ep)),
        dma((nx,)), dma((nx,)), dma((nx - 1, ep)), dma((nx - 1, ep)), dma((ep,)), dma((ep,)),
        dma((tp,)), dma((tp,)), dma((ep,)), dma((ep,)),
    ]
    return pl.pallas_call(
        functools.partial(kernel, ep, tp, cap),
        out_shape=(
            jax.ShapeDtypeStruct((tok_rows, cs), bf16),
            jax.ShapeDtypeStruct(within_ids.shape, f32),
            jax.ShapeDtypeStruct(w_gate.shape, bf16),
            jax.ShapeDtypeStruct(w_up.shape, bf16),
            jax.ShapeDtypeStruct(w_down.shape, bf16),
        ),
        in_specs=[anywhere, anywhere, vmem, vmem, vmem, anywhere, anywhere, anywhere],
        out_specs=(vmem, vmem, anywhere, anywhere, anywhere),
        scratch_shapes=scratch,
        compiler_params=pltpu.CompilerParams(
            collective_id=0, has_side_effects=True, vmem_limit_bytes=56 * 1024 * 1024),
    )(tokens, cotangent, group_ids, within_ids, gate_weights, w_gate, w_up, w_down)


def solution(mesh):
    in_specs = (
        P("ep", None),
        P("ep", None),
        P("ep", None),
        P("ep", None),
        P("ep", None),
        P("ep", None, "tp"),
        P("ep", None, "tp"),
        P("ep", "tp", None),
    )
    out_specs = (
        P("ep", "tp"),
        P("ep", None),
        P("ep", None, "tp"),
        P("ep", None, "tp"),
        P("ep", "tp", None),
    )
    return jax.shard_map(
        on_device, mesh=mesh, in_specs=in_specs, out_specs=out_specs, check_vma=False
    )
```

```python
import functools

import jax
import jax.numpy as jnp
from jax import lax
from jax.experimental import pallas as pl
from jax.experimental.pallas import tpu as pltpu
from jax.sharding import PartitionSpec as P

MESH = pl.DeviceIdType.MESH
LANES = 128
NT = (((1,), (1,)), ((), ()))
TN = (((0,), (0,)), ((), ()))
NN = (((1,), (0,)), ((), ()))


def dot(a, b, dims=NN):
    return lax.dot_general(a, b, dims, preferred_element_type=jnp.float32)


def each(count, body):
    if count <= 8:
        for i in range(count):
            body(i)
    else:
        lax.fori_loop(0, count, lambda i, c: (body(i), c)[1], 0)


def aligned(value, step):
    return value if isinstance(value, int) else pl.multiple_of(value, step)


def kernel(
    ep, tp, cap,
    tok_ref, cot_ref, gid_ref, wid_ref, gw_ref, wg_ref, wu_ref, wd_ref,
    place_ref, back, gate_back, vwg, vwu, vwd,
    src, placed, rows_in, wg, wu, wd, acc, gate_b, up_b, act_c,
    to_partner, from_partner, dx_acc, to_x, from_x, to_ep,
    gate_in, gate_sum,
    load_sem, own_sem, send1, recv_rows, send_x, send_p, send_p2,
    dxp_send, dxp_recv, dxx_send, dxx_recv, dxe_send, dxe_recv,
    gt_send, gt_recv, ge_send, ge_recv,
):
    e_me = lax.axis_index("ep")
    t_me = lax.axis_index("tp")
    core = lax.rem(t_me, 2)
    x_me = lax.div(t_me, 2)
    partner = t_me + 1 - 2 * core
    nx = tp // 2
    tok_rows, width = tok_ref.shape
    cs = width // tp
    slots = ep * cap
    experts = wg.shape[0]
    bf16 = jnp.bfloat16

    barrier = pltpu.get_barrier_semaphore()
    each(ep - 1, lambda i: pl.semaphore_signal(
        barrier, inc=1, device_id=(lax.rem(e_me + 1 + i, ep), t_me), device_id_type=MESH))
    each(tp - 1, lambda i: pl.semaphore_signal(
        barrier, inc=1, device_id=(e_me, lax.rem(t_me + 1 + i, tp)), device_id_type=MESH))

    my_cols = pl.ds(pl.multiple_of(t_me * cs, LANES), cs)
    loads = [
        pltpu.make_async_copy(tok_ref.at[:, my_cols], src.at[:, pl.ds(0, cs)], load_sem.at[0]),
        pltpu.make_async_copy(cot_ref.at[:, my_cols], src.at[:, pl.ds(cs, cs)], load_sem.at[1]),
        pltpu.make_async_copy(wg_ref, wg, load_sem.at[2]),
        pltpu.make_async_copy(wu_ref, wu, load_sem.at[3]),
        pltpu.make_async_copy(wd_ref, wd, load_sem.at[4]),
    ]
    for load in loads:
        load.start()

    group = gid_ref[...]
    groups = -(-ep // 16) * 16
    in_group = (
        lax.broadcasted_iota(jnp.int32, (groups, tok_rows), 0) == group
    ).astype(jnp.float32)
    earlier = (
        lax.broadcasted_iota(jnp.int32, (tok_rows, tok_rows), 0)
        < lax.broadcasted_iota(jnp.int32, (tok_rows, tok_rows), 1)
    ).astype(jnp.float32).astype(bf16)
    before = dot(in_group.astype(bf16), earlier)
    rank = jnp.sum(before * in_group, axis=0, keepdims=True).astype(jnp.int32)
    slot_row = lax.broadcasted_iota(jnp.int32, (slots, tok_rows), 0)
    place = (slot_row == group * cap + rank).astype(jnp.float32).astype(bf16)
    place_ref[0] = place
    place_ref[1] = (slot_row == e_me * cap + rank).astype(jnp.float32).astype(bf16)
    lane_row = lax.broadcasted_iota(jnp.int32, (LANES, tok_rows), 0)
    weights = gw_ref[...].astype(jnp.float32)
    comb = jnp.zeros((LANES, tok_rows), jnp.float32)
    for k in range(weights.shape[0]):
        comb = comb + jnp.where(lane_row == wid_ref[k : k + 1, :], weights[k : k + 1, :], 0.0)
    placed[:, pl.ds(2 * cs, LANES)] = dot(place, comb.astype(bf16), NT).astype(bf16)
    loads[0].wait()
    placed[:, pl.ds(0, cs)] = dot(place, src[:, pl.ds(0, cs)]).astype(bf16)
    loads[1].wait()
    placed[:, pl.ds(cs, cs)] = dot(place, src[:, pl.ds(cs, cs)]).astype(bf16)

    pl.semaphore_wait(barrier, ep + tp - 2)

    def block(e):
        return pl.ds(aligned(e * cap, 16), cap)

    distances = list(range(ep))
    if ep <= 8:
        distances = [0]
        for k in range(1, ep // 2 + 1):
            distances += sorted({k, ep - k})

    def stage1(d):
        g = lax.rem(e_me + d, ep)
        return pltpu.make_async_remote_copy(
            src_ref=placed.at[block(g)], dst_ref=rows_in.at[t_me, block(e_me)],
            send_sem=send1.at[d], recv_sem=recv_rows.at[t_me, e_me],
            device_id=(g, t_me), device_id_type=MESH)

    own = pltpu.make_async_copy(
        placed.at[block(e_me)], rows_in.at[t_me, block(e_me)], own_sem.at[0])
    own.start()
    if ep <= 8:
        for d in distances[1:]:
            stage1(d).start()
    else:
        each(ep - 1, lambda i: stage1(i + 1).start())

    def arrived(q, e, cols):
        part = rows_in.at[q, block(e), pl.ds(0, cols)]
        pltpu.make_async_remote_copy(
            src_ref=part, dst_ref=part, send_sem=send1.at[0], recv_sem=recv_rows.at[q, e],
            device_id=(e_me, partner), device_id_type=MESH).wait_recv()

    def forward(q, e, sem, target):
        part = rows_in.at[q, block(e), pl.ds(0, 2 * cs)]
        return pltpu.make_async_remote_copy(
            src_ref=part, dst_ref=part, send_sem=sem, recv_sem=recv_rows.at[q, e],
            device_id=(e_me, target), device_id_type=MESH)

    def x_peer(k):
        return lax.rem(x_me + k, nx) * 2 + core

    def to_peers(d):
        e = lax.rem(e_me - d + ep, ep)
        copies = [forward(t_me, e, send_x.at[k - 1, d], x_peer(k)) for k in range(1, nx)]
        return copies + [forward(t_me, e, send_p.at[d], partner)]

    def stage2(d):
        for copy in to_peers(d):
            copy.start()

    def relays(d):
        e = lax.rem(e_me - d + ep, ep)
        return [(x_peer(k), e, forward(x_peer(k), e, send_p2.at[k - 1, d], partner))
                for k in range(1, nx)]

    def stage3(d):
        for q, e, copy in relays(d):
            arrived(q, e, 2 * cs)
            copy.start()

    own.wait()
    stage2(0)
    if ep <= 8:
        for i, d in enumerate(distances[1:]):
            arrived(t_me, lax.rem(e_me - d + ep, ep), 2 * cs + LANES)
            stage2(d)
            stage3(distances[i])
    else:
        def later(i):
            arrived(t_me, lax.rem(e_me - i - 1 + ep, ep), 2 * cs + LANES)
            stage2(i + 1)
        each(ep - 1, later)
        each(ep - 1, stage3)

    for load in loads[2:]:
        load.wait()

    def share(q):
        return pl.ds(aligned(q * cs, LANES), cs)

    def hidden(q, first):
        xq = rows_in[q, :, pl.ds(0, cs)]
        yq = rows_in[q, :, pl.ds(cs, cs)]
        for e in range(experts):
            for n, value in enumerate((
                dot(xq, wg[e, share(q), :]),
                dot(xq, wu[e, share(q), :]),
                dot(yq, wd[e, :, share(q)], NT),
            )):
                acc[e, n] = value if first else acc[e, n] + value

    def all_arrived(q):
        each(ep, lambda e: arrived(q, e, 2 * cs))

    hidden(t_me, True)
    stage3(distances[-1])
    all_arrived(partner)
    hidden(partner, False)

    def x_quarters(k):
        hidden(x_peer(k), False)
        other = lax.rem(x_me + k, nx) * 2 + 1 - core
        all_arrived(other)
        hidden(other, False)
    each(nx - 1, lambda i: x_quarters(i + 1))

    row8 = lax.broadcasted_iota(jnp.int32, (8, slots), 0)
    gates = jnp.zeros((8, slots), jnp.float32)
    for e in range(experts):
        pre_gate, pre_up, dy_down = acc[e, 0], acc[e, 1], acc[e, 2]
        c = rows_in[t_me, :, pl.ds(2 * cs, LANES)][:, e : e + 1].astype(jnp.float32)
        sig = jax.nn.sigmoid(pre_gate)
        silu = pre_gate * sig
        act = silu * pre_up
        prod = act.astype(bf16).astype(jnp.float32) * dy_down
        act_grad = c * dy_down
        act_c[e] = (c * act).astype(bf16)
        gate_b[e] = (act_grad * pre_up * sig * (1.0 + pre_gate * (1.0 - sig))).astype(bf16)
        up_b[e] = (act_grad * silu).astype(bf16)
        high = prod.astype(bf16)
        low = (prod - high.astype(jnp.float32)).astype(bf16)
        ones = jnp.ones((8, prod.shape[1]), bf16)
        gates = gates + jnp.where(row8 == e, dot(ones, high, NT) + dot(ones, low, NT), 0.0)
    gate_in[t_me] = gates

    def gate_tp(i):
        return pltpu.make_async_remote_copy(
            src_ref=gate_in.at[t_me], dst_ref=gate_in.at[t_me],
            send_sem=gt_send.at[i], recv_sem=gt_recv.at[t_me],
            device_id=(e_me, lax.rem(t_me + 1 + i, tp)), device_id_type=MESH)

    def dx_of(q):
        total = None
        for e in range(experts):
            part = dot(gate_b[e], wg[e, share(q), :], NT) + dot(up_b[e], wu[e, share(q), :], NT)
            total = part if total is None else total + part
        return total

    def dx_partner(k):
        return pltpu.make_async_remote_copy(
            src_ref=to_partner.at[k], dst_ref=from_partner.at[k],
            send_sem=dxp_send.at[k], recv_sem=dxp_recv.at[k],
            device_id=(e_me, partner), device_id_type=MESH)

    def give_partner(i):
        k = nx - 1 - i
        to_partner[k] = dx_of(lax.rem(x_me + k, nx) * 2 + 1 - core).astype(bf16)
        dx_partner(k).start()
    each(nx, give_partner)
    each(tp - 1, lambda i: gate_tp(i).start())

    def dx_x(k, d):
        e = lax.rem(e_me + d, ep)
        return pltpu.make_async_remote_copy(
            src_ref=to_x.at[k - 1, block(e)], dst_ref=from_x.at[k - 1, block(e)],
            send_sem=dxx_send.at[k - 1, d], recv_sem=dxx_recv.at[k - 1, d],
            device_id=(e_me, x_peer(k)), device_id_type=MESH)

    far = distances[::-1]

    def walk(body):
        if ep <= 8:
            for i, d in enumerate(far):
                body(i, d)
        else:
            each(ep, lambda i: body(i, ep - 1 - i))

    def give_x(k):
        mine = dx_of(x_peer(k))
        dx_partner(k).wait_recv()
        to_x[k - 1] = (mine + from_partner[k].astype(jnp.float32)).astype(bf16)
        walk(lambda i, d: dx_x(k, d).start())
    each(nx - 1, lambda i: give_x(i + 1))
    mine = dx_of(t_me)
    dx_partner(0).wait_recv()
    dx_acc[...] = mine + from_partner[0].astype(jnp.float32)

    def gate_ep(d):
        return pltpu.make_async_remote_copy(
            src_ref=gate_sum, dst_ref=gate_back.at[e_me],
            send_sem=ge_send.at[d], recv_sem=ge_recv.at[e_me],
            device_id=(lax.rem(e_me + d, ep), t_me), device_id_type=MESH)

    def gate_wait(i):
        q = lax.rem(t_me + 1 + i, tp)
        pltpu.make_async_remote_copy(
            src_ref=gate_in.at[q], dst_ref=gate_in.at[q],
            send_sem=gt_send.at[i], recv_sem=gt_recv.at[q],
            device_id=(e_me, q), device_id_type=MESH).wait_recv()
    each(tp - 1, gate_wait)
    total = gate_in[0]
    for q in range(1, tp):
        total = total + gate_in[q]
    gate_sum[...] = total
    gate_back[e_me] = total
    each(ep - 1, lambda i: gate_ep(i + 1).start())

    def weight_grads(q):
        x_t = rows_in[q, :, pl.ds(0, cs)].T
        yq = rows_in[q, :, pl.ds(cs, cs)]
        for e in range(experts):
            vwg[e, share(q), :] = dot(x_t, gate_b[e]).astype(bf16)
            vwu[e, share(q), :] = dot(x_t, up_b[e]).astype(bf16)
            vwd[e, :, share(q)] = dot(act_c[e], yq, TN).astype(bf16)

    def dx_ep(d):
        g = lax.rem(e_me + d, ep)
        return pltpu.make_async_remote_copy(
            src_ref=to_ep.at[block(g)], dst_ref=back.at[block(e_me)],
            send_sem=dxe_send.at[d], recv_sem=dxe_recv.at[e_me],
            device_id=(g, t_me), device_id_type=MESH)

    def finish_chunk(d):
        rows = block(lax.rem(e_me + d, ep))
        value = dx_acc[rows, :]
        for k in range(1, nx):
            dx_x(k, d).wait_recv()
            value = value + from_x[k - 1, rows, :].astype(jnp.float32)
        return value.astype(bf16)

    def chunk(i, d):
        to_ep[block(lax.rem(e_me + d, ep)), :] = finish_chunk(d)
        dx_ep(d).start()

    if ep <= 8:
        done = 0
        for i, d in enumerate(far[:-1]):
            chunk(i, d)
            if i % 2 == 0 and done < tp:
                weight_grads(done)
                done += 1
        for q in range(done, tp):
            weight_grads(q)
    else:
        each(ep - 1, lambda i: chunk(i, ep - 1 - i))
        each(tp, weight_grads)
    back[block(e_me), :] = finish_chunk(0)

    def gate_arrived(i):
        g = lax.rem(e_me + 1 + i, ep)
        pltpu.make_async_remote_copy(
            src_ref=gate_sum, dst_ref=gate_back.at[g],
            send_sem=ge_send.at[0], recv_sem=ge_recv.at[g],
            device_id=(g, t_me), device_id_type=MESH).wait_recv()
    each(ep - 1, gate_arrived)
    def back_arrived(i):
        g = lax.rem(e_me + 1 + i, ep)
        pltpu.make_async_remote_copy(
            src_ref=to_ep.at[block(g)], dst_ref=back.at[block(g)],
            send_sem=dxe_send.at[0], recv_sem=dxe_recv.at[g],
            device_id=(g, t_me), device_id_type=MESH).wait_recv()
    each(ep - 1, back_arrived)

    def sent1(i):
        d = i + 1
        stage1(d).wait_send()
        gate_ep(d).wait_send()
        dx_ep(d).wait_send()
    each(ep - 1, sent1)

    def sent2(d):
        for copy in to_peers(d):
            copy.wait_send()
        for _, _, copy in relays(d):
            copy.wait_send()
        for k in range(1, nx):
            dx_x(k, d).wait_send()
    each(ep, sent2)
    each(nx, lambda k: dx_partner(k).wait_send())
    each(tp - 1, lambda i: gate_tp(i).wait_send())


def finish(
    place_ref, back, gate_back, vwg, vwu, vwd, gid_ref, wid_ref,
    dtok_ref, dgate_ref, gwg_ref, gwu_ref, gwd_ref, sem,
):
    copies = [
        pltpu.make_async_copy(a, b, sem.at[i])
        for i, (a, b) in enumerate(((vwg, gwg_ref), (vwu, gwu_ref), (vwd, gwd_ref)))
    ]
    for copy in copies:
        copy.start()
    ep, _, slots = gate_back.shape
    tok_rows = place_ref.shape[2]
    dtok_ref[...] = dot(place_ref[0], back[...], TN).astype(jnp.bfloat16)
    sums = gate_back[...].reshape(ep * 8, slots)
    high = sums.astype(jnp.bfloat16)
    low = (sums - high.astype(jnp.float32)).astype(jnp.bfloat16)
    dense = dot(high, place_ref[1]) + dot(low, place_ref[1])
    row = lax.broadcasted_iota(jnp.int32, (ep * 8, tok_rows), 0)
    for k in range(wid_ref.shape[0]):
        wanted = row == gid_ref[...] * 8 + wid_ref[k : k + 1, :]
        dgate_ref[k : k + 1, :] = jnp.sum(jnp.where(wanted, dense, 0.0), axis=0, keepdims=True)
    for copy in copies:
        copy.wait()


def on_device(tokens, cotangent, group_ids, within_ids, gate_weights, w_gate, w_up, w_down):
    ep = lax.axis_size("ep")
    tp = lax.axis_size("tp")
    tok_rows, width = tokens.shape
    experts, _, ff = w_gate.shape
    cap = (3 * tok_rows + 2 * ep - 1) // (2 * ep)
    cap = -(-cap // 16) * 16
    slots = ep * cap
    cs = width // tp
    nx = tp // 2
    bf16, f32 = jnp.bfloat16, jnp.float32
    dma = pltpu.SemaphoreType.DMA
    hbm = pl.BlockSpec(memory_space=pltpu.HBM)
    vmem = pl.BlockSpec(memory_space=pltpu.VMEM)
    scratch = [
        pltpu.VMEM((tok_rows, 2 * cs), bf16),
        pltpu.VMEM((slots, 2 * cs + LANES), bf16),
        pltpu.VMEM((tp, slots, 2 * cs + LANES), bf16),
        pltpu.VMEM(w_gate.shape, bf16),
        pltpu.VMEM(w_up.shape, bf16),
        pltpu.VMEM(w_down.shape, bf16),
        pltpu.VMEM((experts, 3, slots, ff), f32),
        pltpu.VMEM((experts, slots, ff), bf16),
        pltpu.VMEM((experts, slots, ff), bf16),
        pltpu.VMEM((experts, slots, ff), bf16),
        pltpu.VMEM((nx, slots, cs), bf16),
        pltpu.VMEM((nx, slots, cs), bf16),
        pltpu.VMEM((slots, cs), f32),
        pltpu.VMEM((nx - 1, slots, cs), bf16),
        pltpu.VMEM((nx - 1, slots, cs), bf16),
        pltpu.VMEM((slots, cs), bf16),
        pltpu.VMEM((tp, 8, slots), f32),
        pltpu.VMEM((8, slots), f32),
        dma((5,)), dma((1,)), dma((ep,)), dma((tp, ep)),
        dma((nx - 1, ep)), dma((ep,)), dma((nx - 1, ep)),
        dma((nx,)), dma((nx,)), dma((nx - 1, ep)), dma((nx - 1, ep)), dma((ep,)), dma((ep,)),
        dma((tp,)), dma((tp,)), dma((ep,)), dma((ep,)),
    ]
    gid, wid, gw = group_ids.T, within_ids.T, gate_weights.T
    kept = pl.pallas_call(
        functools.partial(kernel, ep, tp, cap),
        out_shape=(
            pltpu.VMEM((2, slots, tok_rows), bf16),
            pltpu.VMEM((slots, cs), bf16),
            pltpu.VMEM((ep, 8, slots), f32),
            pltpu.VMEM(w_gate.shape, bf16),
            pltpu.VMEM(w_up.shape, bf16),
            pltpu.VMEM(w_down.shape, bf16),
        ),
        in_specs=[hbm, hbm, vmem, vmem, vmem, hbm, hbm, hbm],
        out_specs=(vmem,) * 6,
        scratch_shapes=scratch,
        compiler_params=pltpu.CompilerParams(
            collective_id=0, has_side_effects=True, vmem_limit_bytes=40 * 1024 * 1024),
    )(tokens, cotangent, gid, wid, gw, w_gate, w_up, w_down)
    dtok, dgate, gwg, gwu, gwd = pl.pallas_call(
        finish,
        out_shape=(
            jax.ShapeDtypeStruct((tok_rows, cs), bf16),
            jax.ShapeDtypeStruct(wid.shape, f32),
            jax.ShapeDtypeStruct(w_gate.shape, bf16),
            jax.ShapeDtypeStruct(w_up.shape, bf16),
            jax.ShapeDtypeStruct(w_down.shape, bf16),
        ),
        in_specs=[vmem] * 8,
        out_specs=(vmem, vmem, hbm, hbm, hbm),
        scratch_shapes=[dma((3,))],
        compiler_params=pltpu.CompilerParams(vmem_limit_bytes=12 * 1024 * 1024),
    )(*kept, gid, wid)
    return dtok, dgate.T, gwg, gwu, gwd


def solution(mesh):
    in_specs = (
        P("ep", None),
        P("ep", None),
        P("ep", None),
        P("ep", None),
        P("ep", None),
        P("ep", None, "tp"),
        P("ep", None, "tp"),
        P("ep", "tp", None),
    )
    out_specs = (
        P("ep", "tp"),
        P("ep", None),
        P("ep", None, "tp"),
        P("ep", None, "tp"),
        P("ep", "tp", None),
    )
    return jax.shard_map(
        on_device, mesh=mesh, in_specs=in_specs, out_specs=out_specs, check_vma=False
    )
```

```python
import functools

import jax
import jax.numpy as jnp
from jax import lax
from jax.experimental import pallas as pl
from jax.experimental.pallas import tpu as pltpu
from jax.sharding import PartitionSpec as P

MESH = pl.DeviceIdType.MESH
LANES = 128
NT = (((1,), (1,)), ((), ()))
TN = (((0,), (0,)), ((), ()))
NN = (((1,), (0,)), ((), ()))


def dot(a, b, dims=NN):
    return lax.dot_general(a, b, dims, preferred_element_type=jnp.float32)


def each(count, body):
    if count <= 8:
        for i in range(count):
            body(i)
    else:
        lax.fori_loop(0, count, lambda i, c: (body(i), c)[1], 0)


def aligned(value, step):
    return value if isinstance(value, int) else pl.multiple_of(value, step)


def kernel(
    ep, tp, cap,
    tok_ref, cot_ref, gid_ref, wid_ref, gw_ref, wg_ref, wu_ref, wd_ref,
    place_ref, back, gate_back, vwg, vwu, vwd,
    src, placed, rows_in, wg, wu, wd, acc, gate_b, up_b, act_c,
    to_partner, from_partner, dx_acc, to_x, from_x, to_ep,
    gate_in, gate_sum,
    load_sem, own_sem, send1, recv_rows, send_x, send_p, send_p2,
    dxp_send, dxp_recv, dxx_send, dxx_recv, dxe_send, dxe_recv,
    gt_send, gt_recv, ge_send, ge_recv,
):
    e_me = lax.axis_index("ep")
    t_me = lax.axis_index("tp")
    core = lax.rem(t_me, 2)
    x_me = lax.div(t_me, 2)
    partner = t_me + 1 - 2 * core
    nx = tp // 2
    gate_lanes = gate_back.shape[2]
    tok_rows, width = tok_ref.shape
    cs = width // tp
    slots = ep * cap
    experts = wg.shape[0]
    bf16 = jnp.bfloat16

    barrier = pltpu.get_barrier_semaphore()
    each(ep - 1, lambda i: pl.semaphore_signal(
        barrier, inc=1, device_id=(lax.rem(e_me + 1 + i, ep), t_me), device_id_type=MESH))
    each(tp - 1, lambda i: pl.semaphore_signal(
        barrier, inc=1, device_id=(e_me, lax.rem(t_me + 1 + i, tp)), device_id_type=MESH))

    my_cols = pl.ds(pl.multiple_of(t_me * cs, LANES), cs)
    loads = [
        pltpu.make_async_copy(tok_ref.at[:, my_cols], src.at[:, pl.ds(0, cs)], load_sem.at[0]),
        pltpu.make_async_copy(cot_ref.at[:, my_cols], src.at[:, pl.ds(cs, cs)], load_sem.at[1]),
        pltpu.make_async_copy(wg_ref, wg, load_sem.at[2]),
        pltpu.make_async_copy(wu_ref, wu, load_sem.at[3]),
        pltpu.make_async_copy(wd_ref, wd, load_sem.at[4]),
    ]
    for load in loads[:2]:
        load.start()

    group = gid_ref[...]
    groups = -(-ep // 16) * 16
    in_group = (
        lax.broadcasted_iota(jnp.int32, (groups, tok_rows), 0) == group
    ).astype(jnp.float32)
    earlier = (
        lax.broadcasted_iota(jnp.int32, (tok_rows, tok_rows), 0)
        < lax.broadcasted_iota(jnp.int32, (tok_rows, tok_rows), 1)
    ).astype(jnp.float32).astype(bf16)
    before = dot(in_group.astype(bf16), earlier)
    rank = jnp.sum(before * in_group, axis=0, keepdims=True).astype(jnp.int32)
    slot_row = lax.broadcasted_iota(jnp.int32, (slots, tok_rows), 0)
    place = (slot_row == group * cap + rank).astype(jnp.float32).astype(bf16)
    place_ref[0] = place
    place_ref[1] = (slot_row == e_me * cap % gate_lanes + rank).astype(jnp.float32).astype(bf16)
    lane_row = lax.broadcasted_iota(jnp.int32, (LANES, tok_rows), 0)
    weights = gw_ref[...].astype(jnp.float32)
    comb = jnp.zeros((LANES, tok_rows), jnp.float32)
    for k in range(weights.shape[0]):
        comb = comb + jnp.where(lane_row == wid_ref[k : k + 1, :], weights[k : k + 1, :], 0.0)
    placed[:, pl.ds(2 * cs, LANES)] = dot(place, comb.astype(bf16), NT).astype(bf16)
    loads[0].wait()
    placed[:, pl.ds(0, cs)] = dot(place, src[:, pl.ds(0, cs)]).astype(bf16)
    loads[1].wait()
    for load in loads[2:]:
        load.start()
    placed[:, pl.ds(cs, cs)] = dot(place, src[:, pl.ds(cs, cs)]).astype(bf16)

    pl.semaphore_wait(barrier, ep + tp - 2)

    def xor(d):
        value, bit = 0, 1
        while bit < ep:
            value = value + (e_me // bit + d // bit) % 2 * bit
            bit *= 2
        return value

    def target(d):
        return xor(d) if ep & (ep - 1) == 0 else lax.rem(e_me + d, ep)

    def source(d):
        return xor(d) if ep & (ep - 1) == 0 else lax.rem(e_me - d + ep, ep)

    def block(e):
        return pl.ds(aligned(e * cap, 16), cap)

    distances = list(range(ep))
    def stage1(d):
        g = target(d)
        return pltpu.make_async_remote_copy(
            src_ref=placed.at[block(g)], dst_ref=rows_in.at[t_me, block(e_me)],
            send_sem=send1.at[d], recv_sem=recv_rows.at[t_me, e_me],
            device_id=(g, t_me), device_id_type=MESH)

    own = pltpu.make_async_copy(
        placed.at[block(e_me)], rows_in.at[t_me, block(e_me)], own_sem.at[0])
    own.start()
    if ep <= 8:
        for d in distances[1:]:
            stage1(d).start()
    else:
        each(ep - 1, lambda i: stage1(i + 1).start())

    def arrived(q, e, cols):
        part = rows_in.at[q, block(e), pl.ds(0, cols)]
        pltpu.make_async_remote_copy(
            src_ref=part, dst_ref=part, send_sem=send1.at[0], recv_sem=recv_rows.at[q, e],
            device_id=(e_me, partner), device_id_type=MESH).wait_recv()

    def forward(q, e, sem, target):
        part = rows_in.at[q, block(e), pl.ds(0, 2 * cs)]
        return pltpu.make_async_remote_copy(
            src_ref=part, dst_ref=part, send_sem=sem, recv_sem=recv_rows.at[q, e],
            device_id=(e_me, target), device_id_type=MESH)

    def x_peer(k):
        return lax.rem(x_me + k, nx) * 2 + core

    def to_peers(d):
        e = source(d)
        copies = [forward(t_me, e, send_x.at[k - 1, d], x_peer(k)) for k in range(1, nx)]
        return copies + [forward(t_me, e, send_p.at[d], partner)]

    def stage2(d):
        for copy in to_peers(d):
            copy.start()

    def relays(d):
        e = source(d)
        return [(x_peer(k), e, forward(x_peer(k), e, send_p2.at[k - 1, d], partner))
                for k in range(1, nx)]

    def stage3(d):
        for q, e, copy in relays(d):
            arrived(q, e, 2 * cs)
            copy.start()

    own.wait()
    stage2(0)
    if ep <= 8:
        for i, d in enumerate(distances[1:]):
            arrived(t_me, source(d), 2 * cs + LANES)
            stage2(d)
    else:
        def later(i):
            arrived(t_me, source(i + 1), 2 * cs + LANES)
            stage2(i + 1)
        each(ep - 1, later)

    for load in loads[2:]:
        load.wait()

    def share(q):
        return pl.ds(aligned(q * cs, LANES), cs)

    def hidden(q, first):
        xq = rows_in[q, :, pl.ds(0, cs)]
        yq = rows_in[q, :, pl.ds(cs, cs)]
        for e in range(experts):
            for n, value in enumerate((
                dot(xq, wg[e, share(q), :]),
                dot(xq, wu[e, share(q), :]),
                dot(yq, wd[e, :, share(q)], NT),
            )):
                acc[e, n] = value if first else acc[e, n] + value

    def all_arrived(q):
        each(ep, lambda e: arrived(q, e, 2 * cs))

    hidden(t_me, True)
    if ep <= 8:
        for d in distances:
            stage3(d)
    else:
        each(ep, stage3)
    all_arrived(partner)
    hidden(partner, False)

    def x_quarters(k):
        hidden(x_peer(k), False)
        other = lax.rem(x_me + k, nx) * 2 + 1 - core
        all_arrived(other)
        hidden(other, False)
    each(nx - 1, lambda i: x_quarters(i + 1))

    row8 = lax.broadcasted_iota(jnp.int32, (8, slots), 0)
    gates = jnp.zeros((8, slots), jnp.float32)
    for e in range(experts):
        pre_gate, pre_up, dy_down = acc[e, 0], acc[e, 1], acc[e, 2]
        c = rows_in[t_me, :, pl.ds(2 * cs, LANES)][:, e : e + 1].astype(jnp.float32)
        sig = jax.nn.sigmoid(pre_gate)
        silu = pre_gate * sig
        act = silu * pre_up
        prod = act.astype(bf16).astype(jnp.float32) * dy_down
        act_grad = c * dy_down
        act_c[e] = (c * act).astype(bf16)
        gate_b[e] = (act_grad * pre_up * sig * (1.0 + pre_gate * (1.0 - sig))).astype(bf16)
        up_b[e] = (act_grad * silu).astype(bf16)
        high = prod.astype(bf16)
        low = (prod - high.astype(jnp.float32)).astype(bf16)
        ones = jnp.ones((8, prod.shape[1]), bf16)
        gates = gates + jnp.where(row8 == e, dot(ones, high, NT) + dot(ones, low, NT), 0.0)
    gate_in[t_me] = gates

    def gate_tp(i):
        return pltpu.make_async_remote_copy(
            src_ref=gate_in.at[t_me], dst_ref=gate_in.at[t_me],
            send_sem=gt_send.at[i], recv_sem=gt_recv.at[t_me],
            device_id=(e_me, lax.rem(t_me + 1 + i, tp)), device_id_type=MESH)

    def dx_of(q):
        total = None
        for e in range(experts):
            part = dot(gate_b[e], wg[e, share(q), :], NT) + dot(up_b[e], wu[e, share(q), :], NT)
            total = part if total is None else total + part
        return total

    def dx_partner(k):
        return pltpu.make_async_remote_copy(
            src_ref=to_partner.at[k], dst_ref=from_partner.at[k],
            send_sem=dxp_send.at[k], recv_sem=dxp_recv.at[k],
            device_id=(e_me, partner), device_id_type=MESH)

    def give_partner(i):
        k = nx - 1 - i
        to_partner[k] = dx_of(lax.rem(x_me + k, nx) * 2 + 1 - core).astype(bf16)
        dx_partner(k).start()

    def dx_x(k, d):
        e = target(d)
        return pltpu.make_async_remote_copy(
            src_ref=to_x.at[k - 1, block(e)], dst_ref=from_x.at[k - 1, block(e)],
            send_sem=dxx_send.at[k - 1, d], recv_sem=dxx_recv.at[k - 1, d],
            device_id=(e_me, x_peer(k)), device_id_type=MESH)

    far = distances[::-1]

    def walk(body):
        if ep <= 8:
            for i, d in enumerate(far):
                body(i, d)
        else:
            each(ep, lambda i: body(i, ep - 1 - i))

    def give_x(k):
        mine = dx_of(x_peer(k))
        dx_partner(k).wait_recv()
        to_x[k - 1] = (mine + from_partner[k].astype(jnp.float32)).astype(bf16)
        walk(lambda i, d: dx_x(k, d).start())
    each(tp - 1, lambda i: gate_tp(i).start())

    def cross(i):
        give_partner(i)
        give_x(nx - 1 - i)
    each(nx - 1, cross)
    give_partner(nx - 1)
    mine = dx_of(t_me)
    dx_partner(0).wait_recv()
    dx_acc[...] = mine + from_partner[0].astype(jnp.float32)

    def gate_tile(e):
        return pl.ds(pl.multiple_of(e * cap // gate_lanes * gate_lanes, LANES), gate_lanes)

    def gate_ep(d):
        return pltpu.make_async_remote_copy(
            src_ref=gate_sum.at[:, gate_tile(target(d))], dst_ref=gate_back.at[e_me],
            send_sem=ge_send.at[d], recv_sem=ge_recv.at[e_me],
            device_id=(target(d), t_me), device_id_type=MESH)

    def gate_wait(i):
        q = lax.rem(t_me + 1 + i, tp)
        pltpu.make_async_remote_copy(
            src_ref=gate_in.at[q], dst_ref=gate_in.at[q],
            send_sem=gt_send.at[i], recv_sem=gt_recv.at[q],
            device_id=(e_me, q), device_id_type=MESH).wait_recv()

    def gates_on():
        each(tp - 1, gate_wait)
        total = gate_in[0]
        for q in range(1, tp):
            total = total + gate_in[q]
        gate_sum[...] = total
        gate_back[e_me] = gate_sum[:, gate_tile(e_me)]
        each(ep - 1, lambda i: gate_ep(i + 1).start())

    def weight_grads(q):
        x_t = rows_in[q, :, pl.ds(0, cs)].T
        yq = rows_in[q, :, pl.ds(cs, cs)]
        for e in range(experts):
            vwg[e, share(q), :] = dot(x_t, gate_b[e]).astype(bf16)
            vwu[e, share(q), :] = dot(x_t, up_b[e]).astype(bf16)
            vwd[e, :, share(q)] = dot(act_c[e], yq, TN).astype(bf16)

    def dx_ep(d):
        g = target(d)
        return pltpu.make_async_remote_copy(
            src_ref=to_ep.at[block(g)], dst_ref=back.at[block(e_me)],
            send_sem=dxe_send.at[d], recv_sem=dxe_recv.at[e_me],
            device_id=(g, t_me), device_id_type=MESH)

    def finish_chunk(d):
        rows = block(target(d))
        value = dx_acc[rows, :]
        for k in range(1, nx):
            dx_x(k, d).wait_recv()
            value = value + from_x[k - 1, rows, :].astype(jnp.float32)
        return value.astype(bf16)

    def chunk(i, d):
        to_ep[block(target(d)), :] = finish_chunk(d)
        dx_ep(d).start()

    if ep <= 8:
        done = 0
        for i, d in enumerate(far[:-1]):
            chunk(i, d)
            if i % 2 == 0 and done < tp:
                weight_grads(done)
                done += 1
            if i == min(2, ep - 2):
                gates_on()
        for q in range(done, tp):
            weight_grads(q)
    else:
        each(ep - 1, lambda i: chunk(i, ep - 1 - i))
        each(tp, weight_grads)
        gates_on()
    back[block(e_me), :] = finish_chunk(0)

    def gate_arrived(i):
        g = lax.rem(e_me + 1 + i, ep)
        pltpu.make_async_remote_copy(
            src_ref=gate_sum.at[:, gate_tile(g)], dst_ref=gate_back.at[g],
            send_sem=ge_send.at[0], recv_sem=ge_recv.at[g],
            device_id=(g, t_me), device_id_type=MESH).wait_recv()
    each(ep - 1, gate_arrived)
    def back_arrived(i):
        g = lax.rem(e_me + 1 + i, ep)
        pltpu.make_async_remote_copy(
            src_ref=to_ep.at[block(g)], dst_ref=back.at[block(g)],
            send_sem=dxe_send.at[0], recv_sem=dxe_recv.at[g],
            device_id=(g, t_me), device_id_type=MESH).wait_recv()
    each(ep - 1, back_arrived)

    def sent1(i):
        d = i + 1
        stage1(d).wait_send()
        gate_ep(d).wait_send()
        dx_ep(d).wait_send()
    each(ep - 1, sent1)

    def sent2(d):
        for copy in to_peers(d):
            copy.wait_send()
        for _, _, copy in relays(d):
            copy.wait_send()
        for k in range(1, nx):
            dx_x(k, d).wait_send()
    each(ep, sent2)
    each(nx, lambda k: dx_partner(k).wait_send())
    each(tp - 1, lambda i: gate_tp(i).wait_send())


def finish(
    place_ref, back, gate_back, vwg, vwu, vwd, gid_ref, wid_ref,
    dtok_ref, dgate_ref, gwg_ref, gwu_ref, gwd_ref, dtok, dgate, sem,
):
    copies = []
    for a, b in ((vwg, gwg_ref), (vwu, gwu_ref), (vwd, gwd_ref)):
        experts, rows, _ = a.shape
        for e in range(experts):
            for half in range(2):
                part = pl.ds(half * (rows // 2), rows // 2)
                copies.append(pltpu.make_async_copy(
                    a.at[e, part], b.at[e, part], sem.at[2 + len(copies)]))
    for copy in copies:
        copy.start()
    ep, _, slots = gate_back.shape
    tok_rows = place_ref.shape[2]
    dtok[...] = dot(place_ref[0], back[...], TN).astype(jnp.bfloat16)
    copies.append(pltpu.make_async_copy(dtok, dtok_ref, sem.at[0]))
    copies[-1].start()
    sums = gate_back[...].reshape(ep * 8, slots)
    high = sums.astype(jnp.bfloat16)
    low = (sums - high.astype(jnp.float32)).astype(jnp.bfloat16)
    pick = place_ref[1, :slots, :]
    dense = dot(high, pick) + dot(low, pick)
    row = lax.broadcasted_iota(jnp.int32, (ep * 8, tok_rows), 0)
    for k in range(wid_ref.shape[0]):
        wanted = row == gid_ref[...] * 8 + wid_ref[k : k + 1, :]
        dgate[k : k + 1, :] = jnp.sum(jnp.where(wanted, dense, 0.0), axis=0, keepdims=True)
    copies.append(pltpu.make_async_copy(dgate, dgate_ref, sem.at[1]))
    copies[-1].start()
    for copy in copies:
        copy.wait()


def on_device(tokens, cotangent, group_ids, within_ids, gate_weights, w_gate, w_up, w_down):
    ep = lax.axis_size("ep")
    tp = lax.axis_size("tp")
    tok_rows, width = tokens.shape
    experts, _, ff = w_gate.shape
    cap = (3 * tok_rows + 2 * ep - 1) // (2 * ep)
    cap = -(-cap // 16) * 16
    slots = ep * cap
    gate_lanes = LANES if LANES % cap == 0 and slots % LANES == 0 else slots
    cs = width // tp
    nx = tp // 2
    bf16, f32 = jnp.bfloat16, jnp.float32
    dma = pltpu.SemaphoreType.DMA
    hbm = pl.BlockSpec(memory_space=pltpu.HBM)
    vmem = pl.BlockSpec(memory_space=pltpu.VMEM)
    scratch = [
        pltpu.VMEM((tok_rows, 2 * cs), bf16),
        pltpu.VMEM((slots, 2 * cs + LANES), bf16),
        pltpu.VMEM((tp, slots, 2 * cs + LANES), bf16),
        pltpu.VMEM(w_gate.shape, bf16),
        pltpu.VMEM(w_up.shape, bf16),
        pltpu.VMEM(w_down.shape, bf16),
        pltpu.VMEM((experts, 3, slots, ff), f32),
        pltpu.VMEM((experts, slots, ff), bf16),
        pltpu.VMEM((experts, slots, ff), bf16),
        pltpu.VMEM((experts, slots, ff), bf16),
        pltpu.VMEM((nx, slots, cs), bf16),
        pltpu.VMEM((nx, slots, cs), bf16),
        pltpu.VMEM((slots, cs), f32),
        pltpu.VMEM((nx - 1, slots, cs), bf16),
        pltpu.VMEM((nx - 1, slots, cs), bf16),
        pltpu.VMEM((slots, cs), bf16),
        pltpu.VMEM((tp, 8, slots), f32),
        pltpu.VMEM((8, slots), f32),
        dma((5,)), dma((1,)), dma((ep,)), dma((tp, ep)),
        dma((nx - 1, ep)), dma((ep,)), dma((nx - 1, ep)),
        dma((nx,)), dma((nx,)), dma((nx - 1, ep)), dma((nx - 1, ep)), dma((ep,)), dma((ep,)),
        dma((tp,)), dma((tp,)), dma((ep,)), dma((ep,)),
    ]
    gid, wid, gw = group_ids.T, within_ids.T, gate_weights.T
    kept = pl.pallas_call(
        functools.partial(kernel, ep, tp, cap),
        out_shape=(
            pltpu.VMEM((2, slots, tok_rows), bf16),
            pltpu.VMEM((slots, cs), bf16),
            pltpu.VMEM((ep, 8, gate_lanes), f32),
            pltpu.VMEM(w_gate.shape, bf16),
            pltpu.VMEM(w_up.shape, bf16),
            pltpu.VMEM(w_down.shape, bf16),
        ),
        in_specs=[hbm, hbm, vmem, vmem, vmem, hbm, hbm, hbm],
        out_specs=(vmem,) * 6,
        scratch_shapes=scratch,
        compiler_params=pltpu.CompilerParams(
            collective_id=0, has_side_effects=True, vmem_limit_bytes=57 * 1024 * 1024),
    )(tokens, cotangent, gid, wid, gw, w_gate, w_up, w_down)
    dtok, dgate, gwg, gwu, gwd = pl.pallas_call(
        finish,
        out_shape=(
            jax.ShapeDtypeStruct((tok_rows, cs), bf16),
            jax.ShapeDtypeStruct(wid.shape, f32),
            jax.ShapeDtypeStruct(w_gate.shape, bf16),
            jax.ShapeDtypeStruct(w_up.shape, bf16),
            jax.ShapeDtypeStruct(w_down.shape, bf16),
        ),
        in_specs=[vmem] * 8,
        out_specs=(hbm,) * 5,
        scratch_shapes=[
            pltpu.VMEM((tok_rows, cs), bf16),
            pltpu.VMEM(wid.shape, f32),
            dma((2 + 6 * experts,)),
        ],
        compiler_params=pltpu.CompilerParams(vmem_limit_bytes=12 * 1024 * 1024),
    )(*kept, gid, wid)
    return dtok, dgate.T, gwg, gwu, gwd


def solution(mesh):
    in_specs = (
        P("ep", None),
        P("ep", None),
        P("ep", None),
        P("ep", None),
        P("ep", None),
        P("ep", None, "tp"),
        P("ep", None, "tp"),
        P("ep", "tp", None),
    )
    out_specs = (
        P("ep", "tp"),
        P("ep", None),
        P("ep", None, "tp"),
        P("ep", None, "tp"),
        P("ep", "tp", None),
    )
    return jax.shard_map(
        on_device, mesh=mesh, in_specs=in_specs, out_specs=out_specs, check_vma=False
    )
```
